32 devices in a mesh: ep: 8 (over z, x), tp: 4 (over y, core).
Axes of the slice: x: 2, y: 2, z: 4, core: 2. Of those that a mesh axis runs over, the one named last changes fastest.
Arguments:
- queries: bfloat16 [4096, 2048], P('ep', 'tp'), may hold values from -5 to 5
- key_rows: bfloat16 [4096, 2048], P('ep', 'tp'), may hold values from -5 to 5
- values: bfloat16 [4096, 2048], P('ep', 'tp'), may hold values from -6 to 6
- forget_log: float32 [4096, 16], P(None, 'tp'), may hold values from -515 to 0, as said below
- out_weight: bfloat16 [2048, 4096], P(None, 'tp'), may hold values from -1 to 1
- expert_input: bfloat16 [1024, 4096], P(('ep', 'tp')), may hold values from -6 to 6
- norm_gain: float32 [4096], replicated, may hold values from 0.1 to 1.9
- route_ids: int32 [1024, 2], P('ep'), may hold values from 0 to 7, all different within a row; in each aligned block of 128 rows (0 to 127, 128 to 255, ...) at most 64 rows name the same one
- route_weights: float32 [1024, 2], P('ep'), may hold values from 0.2 to 1
- gate_weight: bfloat16 [8, 4096, 2048], P('ep', None, 'tp'), may hold values from -0.09375 to 0.09375
- up_weight: bfloat16 [8, 4096, 2048], P('ep', None, 'tp'), may hold values from -0.09375 to 0.09375
- down_weight: bfloat16 [8, 2048, 4096], P('ep', None, 'tp'), may hold values from -0.125 to 0.125
Outputs:
- mixer_out: bfloat16 [4096, 4096], P('ep', 'tp')
- expert_out: bfloat16 [1024, 4096], P('ep', 'tp')
The draws below stay inside these ranges and needn't reach their ends.
Inputs may be any that keep to these rules, and one draw needn't show every extreme that they name: forget_log[t, h] is the sum of the log forget gates of head h at positions 0 to t of the one sequence; it never rises along positions. `route_ids`: each row names 2 different experts. In each aligned block of 128 rows (the rows of one index of ep) no expert is named by more than 64 rows, and some block reaches 64.
All inputs are finite; a program needn't handle non-finite values.
Results may differ from the reference program's by a relative error of at most 0.0071.
Values may be sent and summed in bfloat16 or wider, within the bound.
A program may use at most 64 MiB of HBM per device.

```python
import math
import jax
import jax.numpy as jnp
import numpy as np
from jax import lax

D = 4096
HEAD_COUNT = 16
HD = 128
FFE = 2048
TOPK = 2
ROWS_A = 512
ROWS_B = 128
SEQUENCE_LENGTH = 4096
TOKENS_B = 1024
EXPERTS = 8
CAP = 64
N_EP = 8


def draw_queries(key, part):
    drawn_rows = jnp.clip(1.5 * jax.random.normal(jax.random.fold_in(key, 1), (SEQUENCE_LENGTH, HEAD_COUNT * HD), jnp.float32), -5.0, 5.0)
    return drawn_rows.astype(jnp.bfloat16)


def draw_key_rows(key, part):
    drawn_rows = jnp.clip(jax.random.normal(jax.random.fold_in(key, 2), (SEQUENCE_LENGTH, HEAD_COUNT * HD), jnp.float32), -5.0, 5.0)
    return drawn_rows.astype(jnp.bfloat16)


def draw_forget_log(key, part):
    fast_share = 0.5
    fast_heads = jax.random.uniform(jax.random.fold_in(key, 3), (HEAD_COUNT,), jnp.float32) < fast_share
    slow_rate = jnp.exp(jax.random.uniform(jax.random.fold_in(key, 4), (HEAD_COUNT,), jnp.float32, jnp.log(0.2), jnp.log(0.8))) / SEQUENCE_LENGTH
    fast_rate = jnp.exp(jax.random.uniform(jax.random.fold_in(key, 5), (HEAD_COUNT,), jnp.float32, jnp.log(0.01), jnp.log(1.0 / 30.0)))
    head_rate = jnp.where(fast_heads, fast_rate, slow_rate)
    block_factor = jnp.exp(jax.random.uniform(jax.random.fold_in(key, 6), (SEQUENCE_LENGTH // ROWS_A, HEAD_COUNT), jnp.float32, -0.7, 0.7))
    block_factor = jnp.repeat(block_factor, ROWS_A, axis=0)
    roughness = jax.random.uniform(jax.random.fold_in(key, 7), (SEQUENCE_LENGTH, HEAD_COUNT), jnp.float32, 0.3, 1.7)
    step_logarithm = -head_rate[None, :] * block_factor * roughness
    surge_locations = jax.random.randint(jax.random.fold_in(key, 8), (2, HEAD_COUNT), 0, SEQUENCE_LENGTH)
    position_indices = jnp.arange(SEQUENCE_LENGTH, dtype=jnp.int32)
    surge_matched = jnp.any(position_indices[:, None, None] == surge_locations[None, :, :], axis=1)
    surge_penalty = jnp.log(jax.random.uniform(jax.random.fold_in(key, 9), (SEQUENCE_LENGTH, HEAD_COUNT), jnp.float32, 0.6, 0.8))
    step_logarithm = step_logarithm + jnp.where(surge_matched, surge_penalty, 0.0)
    return jnp.cumsum(step_logarithm, axis=0).astype(jnp.float32)


def block_scale(rng, extent, split, least, top_value):
    factor_of, own = 1.0, jax.random.fold_in(rng, 6)
    for dim, shards_of in split:
        draws = jnp.exp(jax.random.uniform(jax.random.fold_in(own, dim), (shards_of,), jnp.float32, least / len(split), top_value / len(split)))
        factor_of = factor_of * jnp.repeat(draws, extent[dim] // shards_of).reshape([-1 if axis == dim else 1 for axis in range(len(extent))])
    return factor_of


def shared_out(rng, own, number, rows, number_of, top, reach, skew):
    order = jax.random.permutation(rng, number_of)
    heavy_load, usual = load_shares(number_of, rows * top, reach, skew, True), load_shares(number_of, rows * top, reach, skew, False)
    places = jnp.arange(number_of)

    def named(sizes, offset_by):
        used = int((sizes > 0).sum())
        fixed = max(1, used // 4)
        passed = fixed + (places - fixed + offset_by * (used - fixed)) % max(1, number_of - fixed)
        return jnp.zeros((number_of,), jnp.int32).at[order[jnp.where(places < fixed, places, passed)]].set(jnp.asarray(sizes, jnp.int32))

    sizes = jnp.where(number % 4 == 0, named(heavy_load, number // 4), named(usual, number - number // 4 - 1))
    mixed = jax.random.permutation(jax.random.fold_in(own, 3), number_of)
    giver, receiver = mixed[0:number_of // 2 * 2:2], mixed[1:number_of // 2 * 2:2]
    slack = jnp.minimum(sizes[giver] - 1, reach - sizes[receiver]) // 2
    slack = jnp.where((giver == order[0]) | (receiver == order[0]) | (sizes[receiver] == 0), 0, jnp.maximum(slack, 0))
    passed = jax.random.randint(jax.random.fold_in(own, 4), (number_of // 2,), 0, 1 << 20) % (slack + 1)
    sizes = sizes.at[giver].add(-passed).at[receiver].add(passed)
    items = jnp.searchsorted(jnp.cumsum(sizes), jnp.arange(rows * top), side="right").astype(jnp.int32)
    table = items.reshape(top, rows).T
    table = table[jax.random.permutation(jax.random.fold_in(own, 1), rows)]
    offset_by = jax.random.randint(jax.random.fold_in(own, 2), (rows, 1), 0, top)
    return jnp.take_along_axis(table, (jnp.arange(top)[None, :] + offset_by) % top, axis=1)


def load_shares(count, total, limit, slope, full):
    portions = [(1 << 20) // math.isqrt(grade ** slope) + 1 for grade in range(1, count + 1)]
    largest = limit if full else min(limit, max(-(-total // count), total * portions[0] // sum(portions)))
    least = 1 if total - largest >= count - 1 else 0
    counts, rest = [largest] + [least] * (count - 1), total - largest - least * (count - 1)
    while rest > 0:
        movable = [i for i in range(1, count) if counts[i] < largest] or [i for i in range(1, count) if counts[i] < limit]
        mass, left = sum([portions[i] for i in movable]), rest
        for i in movable:
            addition = min(limit - counts[i], max(1, left * portions[i] // mass), rest)
            counts[i] = counts[i] + addition
            rest = rest - addition
    return np.array(counts)


def noise(key, dims, width, most, cuts=(), held_as=jnp.bfloat16):
    factor_of = block_scale(key, dims, cuts, -0.22, 0.18) if cuts else 1.0
    drawn = jax.random.normal(key, dims, jnp.float32) * width * factor_of
    return jnp.minimum(jnp.maximum(drawn, -most), most).astype(held_as)


def setup_inputs(seed: int = 0) -> dict:
    key_list = jax.random.split(jax.random.key(seed), 13)
    queries = draw_queries(jax.random.fold_in(key_list[12], 71), 0)
    key_rows = draw_key_rows(jax.random.fold_in(key_list[12], 71), 0)
    values = noise(key_list[2], (SEQUENCE_LENGTH, HEAD_COUNT * HD), 1.0, 6.0, ((0, 8), (1, 4)))
    forget_log = draw_forget_log(jax.random.fold_in(key_list[12], 71), 0)
    out_weight = noise(key_list[4], (HEAD_COUNT * HD, D), (HD // 4) ** -0.5, 1.0, ((1, 4),))
    expert_input = noise(key_list[5], (TOKENS_B, D), 1.0, 6.0, ((0, 32),))
    norm_gain = jnp.clip(1.0 + 0.18 * jax.random.normal(key_list[6], (D,), jnp.float32), 0.1, 1.9)
    route_ids_keys = jax.random.split(jax.random.fold_in(key_list[7], 1), TOKENS_B // ROWS_B)
    route_ids_turns = jax.random.permutation(jax.random.fold_in(key_list[7], 3), TOKENS_B // ROWS_B)
    route_ids = jax.vmap(lambda own, number: shared_out(jax.random.fold_in(key_list[7], 2), own, number, ROWS_B, EXPERTS, TOPK, CAP, 2))(route_ids_keys, route_ids_turns).reshape((TOKENS_B, TOPK))
    route_weights = jnp.clip(0.2 + 0.8 * jax.random.uniform(key_list[8], (TOKENS_B, TOPK), jnp.float32) ** block_scale(key_list[8], (TOKENS_B, TOPK), ((0, 8),), -0.2, 0.2), 0.2, 1.0)
    gate_weight = noise(key_list[9], (EXPERTS, D, FFE), D ** -0.5, 0.09375, ((0, 8), (2, 4)))
    up_weight = noise(key_list[10], (EXPERTS, D, FFE), D ** -0.5, 0.09375, ((0, 8), (2, 4)))
    down_weight = noise(key_list[11], (EXPERTS, FFE, D), FFE ** -0.5, 0.125, ((0, 8), (2, 4)))
    return {"queries": queries, "key_rows": key_rows, "values": values, "forget_log": forget_log, "out_weight": out_weight, "expert_input": expert_input, "norm_gain": norm_gain, "route_ids": route_ids, "route_weights": route_weights, "gate_weight": gate_weight, "up_weight": up_weight, "down_weight": down_weight}


EPSILON = 1e-05

def slot_places(route_rows, experts, capacity):
    entries = route_rows.reshape(-1).astype(jnp.int32)
    matches = (entries[:, None] == jnp.arange(experts, dtype=jnp.int32)[None, :]).astype(jnp.int32)
    earlier = (jnp.cumsum(matches, axis=0) - matches).astype(jnp.int32)
    ranking = lax.optimization_barrier(jnp.sum(earlier * matches, axis=1)).astype(jnp.int32)
    return (entries * capacity + ranking).astype(jnp.int32)

def reference(queries, key_rows, values, forget_log, out_weight, expert_input, norm_gain, route_ids, route_weights, gate_weight, up_weight, down_weight):
    length_all = queries.shape[0]
    query_heads = queries.reshape(length_all, HEAD_COUNT, HD).astype(jnp.float32)
    key_heads = key_rows.reshape(length_all, HEAD_COUNT, HD).astype(jnp.float32)
    value_heads = values.reshape(length_all, HEAD_COUNT, HD).astype(jnp.float32)
    key_places = jnp.arange(length_all, dtype=jnp.int32)
    score_scale = HD ** (-0.5)

    def attend(block_index):
        block_start = (block_index * ROWS_A).astype(jnp.int32)
        query_block = lax.dynamic_slice_in_dim(query_heads, block_start, ROWS_A, 0)
        gate_block = lax.dynamic_slice_in_dim(forget_log, block_start, ROWS_A, 0)
        scores = jnp.einsum('qhd,khd->hqk', query_block, key_heads) * score_scale
        scores = scores + gate_block.T[:, :, None] - forget_log.T[:, None, :]
        query_places = block_start + jnp.arange(ROWS_A, dtype=jnp.int32)
        scores = jnp.where(key_places[None, None, :] <= query_places[None, :, None], scores, -jnp.inf)
        row_max = lax.optimization_barrier(jnp.max(scores, axis=2, keepdims=True))
        weights_now = jnp.exp(scores - row_max)
        denominator = lax.optimization_barrier(jnp.sum(weights_now, axis=2))
        rounded = lax.optimization_barrier(weights_now.astype(jnp.bfloat16)).astype(jnp.float32)
        numerator = jnp.einsum('hqk,khd->qhd', rounded, value_heads)
        return (numerator / denominator.T[:, :, None]).astype(jnp.bfloat16)
    attended = lax.map(attend, jnp.arange(length_all // ROWS_A, dtype=jnp.int32)).reshape(length_all, HEAD_COUNT * HD)
    mixer_out = jnp.dot(attended, out_weight, preferred_element_type=jnp.float32).astype(jnp.bfloat16)
    as_float = expert_input.astype(jnp.float32)
    center = lax.optimization_barrier(jnp.mean(as_float, axis=1, keepdims=True))
    variance = lax.optimization_barrier(jnp.mean(jnp.square(as_float - center), axis=1, keepdims=True))
    normed = ((as_float - center) * lax.rsqrt(variance + EPSILON) * norm_gain).astype(jnp.bfloat16)
    blocks = route_ids.reshape(N_EP, ROWS_B, TOPK)
    places = jax.vmap(lambda block_ids: slot_places(block_ids, EXPERTS, CAP))(blocks)
    expert_of = blocks.reshape(N_EP, ROWS_B * TOPK).astype(jnp.int32)
    ranking = places - expert_of * CAP
    block_index = jnp.arange(N_EP, dtype=jnp.int32)[:, None]
    global_slot = (expert_of * (N_EP * CAP) + block_index * CAP + ranking).astype(jnp.int32)
    owners = (block_index * ROWS_B + jnp.arange(ROWS_B * TOPK, dtype=jnp.int32)[None, :] // TOPK).astype(jnp.int32)
    slot_table = jnp.full((EXPERTS * N_EP * CAP,), TOKENS_B, jnp.int32).at[global_slot.reshape(-1)].set(owners.reshape(-1))
    slot_table = slot_table.reshape(EXPERTS, N_EP * CAP)

    def run_expert(expert_index):
        chosen_rows = jnp.take(normed, slot_table[expert_index], axis=0, mode='fill', fill_value=0)
        gate_part = jnp.dot(chosen_rows, gate_weight[expert_index], preferred_element_type=jnp.float32)
        up_part = jnp.dot(chosen_rows, up_weight[expert_index], preferred_element_type=jnp.float32)
        hidden = (jax.nn.silu(gate_part) * up_part).astype(jnp.bfloat16)
        return jnp.dot(hidden, down_weight[expert_index], preferred_element_type=jnp.float32).astype(jnp.bfloat16)
    results = lax.map(run_expert, jnp.arange(EXPERTS, dtype=jnp.int32)).reshape(EXPERTS * N_EP * CAP, D)
    picked = jnp.take(results, global_slot.reshape(-1), axis=0).astype(jnp.float32)
    combined = lax.optimization_barrier(jnp.sum((picked * route_weights.reshape(-1)[:, None]).reshape(TOKENS_B, TOPK, D), axis=1))
    return (mixer_out, combined.astype(jnp.bfloat16))
```

```python
import functools
import math

import jax
import jax.numpy as jnp
from jax import lax
from jax.experimental import pallas as pl
from jax.experimental.pallas import tpu as pltpu
from jax.sharding import PartitionSpec as P

EPSILON = 1e-05
LOG2E = math.log2(math.e)


def attention_kernel(
    n, heads, gate_row, gate_col, q_ref, k_ref, v_ref, out_ref,
    k_buf, v_buf, q_buf, o_buf,
    recv_k, recv_v, recv_q, recv_o, send_k, send_v, send_q, send_o, pass_k, pass_v,
):
    members = n // heads
    rows = k_ref.shape[0]
    width = k_ref.shape[1] // heads
    chunk = rows // members
    me = lax.axis_index("ep")
    my_member = me % members
    my_head = me // members

    barrier = pltpu.get_barrier_semaphore()

    @pl.loop(1, n)
    def _(step):
        pl.semaphore_signal(barrier, inc=1, device_id={"ep": (me + step) % n})

    pl.semaphore_wait(barrier, n - 1)

    def k_copy(target, head):
        cols = pl.ds(pl.multiple_of(head * width, width), width)
        return pltpu.make_async_remote_copy(
            src_ref=k_ref.at[:, cols], dst_ref=k_buf.at[me], send_sem=send_k.at[head],
            recv_sem=recv_k.at[me], device_id={"ep": target},
        )

    def v_copy(target, head):
        cols = pl.ds(pl.multiple_of(head * width, width), width)
        return pltpu.make_async_remote_copy(
            src_ref=v_ref.at[:, cols], dst_ref=v_buf.at[me], send_sem=send_v.at[head],
            recv_sem=recv_v.at[me], device_id={"ep": target},
        )

    def q_copy(target):
        cols = pl.ds(pl.multiple_of((target // members) * width, width), width)
        part = pl.ds(pl.multiple_of((target % members) * chunk, chunk), chunk)
        return pltpu.make_async_remote_copy(
            src_ref=q_ref.at[part, cols], dst_ref=q_buf.at[me], send_sem=send_q.at[target],
            recv_sem=recv_q.at[me], device_id={"ep": target},
        )

    def pass_copies(source, target):
        return (
            pltpu.make_async_remote_copy(
                src_ref=k_buf.at[source], dst_ref=k_buf.at[source],
                send_sem=pass_k.at[source, target % members],
                recv_sem=recv_k.at[source], device_id={"ep": target},
            ),
            pltpu.make_async_remote_copy(
                src_ref=v_buf.at[source], dst_ref=v_buf.at[source],
                send_sem=pass_v.at[source, target % members],
                recv_sem=recv_v.at[source], device_id={"ep": target},
            ),
        )

    def back_copy(source):
        cols = pl.ds(pl.multiple_of(my_head * width, width), width)
        part = pl.ds(pl.multiple_of(my_member * chunk, chunk), chunk)
        return pltpu.make_async_remote_copy(
            src_ref=o_buf.at[source], dst_ref=out_ref.at[part, cols], send_sem=send_o.at[source],
            recv_sem=recv_o.at[me], device_id={"ep": source},
        )

    own_cols = pl.ds(pl.multiple_of(my_head * width, width), width)
    own_part = pl.ds(pl.multiple_of(my_member * chunk, chunk), chunk)
    pltpu.make_async_copy(k_ref.at[:, own_cols], k_buf.at[me], recv_k.at[me]).start()
    pltpu.make_async_copy(v_ref.at[:, own_cols], v_buf.at[me], recv_v.at[me]).start()
    pltpu.make_async_copy(q_ref.at[own_part, own_cols], q_buf.at[me], recv_q.at[me]).start()

    @pl.loop(1, heads)
    def _(step):
        head = (my_head + step) % heads
        k_copy(head * members + my_member, head).start()
        v_copy(head * members + my_member, head).start()

    @pl.loop(1, n)
    def _(step):
        q_copy((me + step) % n).start()

    def landed(source):
        pltpu.make_async_copy(k_buf.at[source], k_buf.at[source], recv_k.at[source]).wait()
        pltpu.make_async_copy(v_buf.at[source], v_buf.at[source], recv_v.at[source]).wait()

    @pl.loop(0, heads)
    def _(step):
        source = ((my_head + step) % heads) * members + my_member
        landed(source)

        @pl.loop(1, members)
        def _(other):
            for copy in pass_copies(source, my_head * members + (my_member + other) % members):
                copy.start()

    column = lax.broadcasted_iota(jnp.int32, (chunk, rows), 1)
    line = lax.broadcasted_iota(jnp.int32, (chunk, rows), 0) + my_member * chunk
    causal = column <= line
    factor = LOG2E * width ** (-0.5)

    @pl.loop(0, n)
    def _(i):
        pltpu.make_async_copy(q_buf.at[i], q_buf.at[i], recv_q.at[i]).wait()

        @pl.when(i % members != my_member)
        def _():
            landed(i)

        query = q_buf[i]
        line_gate = gate_col[i]

        def scores_of(j):
            raw = lax.dot_general(
                query, k_buf[j], (((1,), (1,)), ((), ())), preferred_element_type=jnp.float32
            )
            return raw * factor + (line_gate - gate_row[j])

        def weigh(weights, j):
            return jnp.dot(
                weights.astype(jnp.bfloat16), v_buf[j], preferred_element_type=jnp.float32
            )

        scores = jnp.where(causal, scores_of(i), -jnp.inf)
        top = jnp.max(scores, axis=1, keepdims=True)
        weights = jnp.exp2(scores - top)
        total = jnp.sum(weights, axis=1, keepdims=True)
        held = weigh(weights, i)

        def fold(j, state):
            top, total, held = state
            scores = scores_of(j)
            newest = jnp.maximum(top, jnp.max(scores, axis=1, keepdims=True))
            shrink = jnp.exp2(top - newest)
            weights = jnp.exp2(scores - newest)
            total = total * shrink + jnp.sum(weights, axis=1, keepdims=True)
            held = held * shrink + weigh(weights, j)
            return newest, total, held

        top, total, held = lax.fori_loop(0, i, fold, (top, total, held))
        o_buf[i] = (held / total).astype(o_buf.dtype)

        @pl.when(i != me)
        def _():
            back_copy(i).start()

    own = pltpu.make_async_copy(o_buf.at[me], out_ref.at[own_part, own_cols], recv_o.at[me])
    own.start()

    @pl.loop(1, heads)
    def _(step):
        head = (my_head + step) % heads
        k_copy(head * members + my_member, head).wait_send()
        v_copy(head * members + my_member, head).wait_send()

    @pl.loop(1, n)
    def _(step):
        q_copy((me + step) % n).wait_send()
        back_copy((me + step) % n).wait_send()

    @pl.loop(0, heads)
    def _(step):
        source = step * members + my_member

        @pl.loop(1, members)
        def _(other):
            for copy in pass_copies(source, my_head * members + (my_member + other) % members):
                copy.wait_send()

    @pl.loop(0, n)
    def _(i):
        cols = pl.ds(pl.multiple_of((i // members) * width, width), width)
        part = pl.ds(pl.multiple_of((i % members) * chunk, chunk), chunk)
        spot = out_ref.at[part, cols]
        pltpu.make_async_copy(spot, spot, recv_o.at[i]).wait()


def attention(queries, key_rows, values, forget_log):
    n = lax.axis_size("ep")
    rows, heads = queries.shape[0], forget_log.shape[1]
    width = queries.shape[1] // heads
    members = n // heads
    chunk = rows // members
    me = lax.axis_index("ep")
    gates = lax.dynamic_slice_in_dim(forget_log.T * LOG2E, me // members, 1, 0)
    gate_row = gates.reshape(n, 1, rows)
    gate_col = lax.dynamic_slice_in_dim(
        gates.reshape(n, members, chunk), me % members, 1, 1
    ).reshape(n, chunk, 1)
    vmem = pl.BlockSpec(memory_space=pltpu.VMEM)
    dma = pltpu.SemaphoreType.DMA
    blocks = n * (n + 1) // 2
    return pl.pallas_call(
        functools.partial(attention_kernel, n, heads),
        out_shape=jax.ShapeDtypeStruct((rows, heads * width), jnp.bfloat16),
        in_specs=[vmem] * 5,
        out_specs=vmem,
        scratch_shapes=[
            pltpu.VMEM((n, rows, width), jnp.bfloat16),
            pltpu.VMEM((n, rows, width), jnp.bfloat16),
            pltpu.VMEM((n, chunk, width), jnp.bfloat16),
            pltpu.VMEM((n, chunk, width), jnp.bfloat16),
            dma((n,)), dma((n,)), dma((n,)), dma((n,)),
            dma((heads,)), dma((heads,)), dma((n,)), dma((n,)),
            dma((n, members)), dma((n, members)),
        ],
        compiler_params=pltpu.CompilerParams(
            collective_id=0, has_side_effects=True, vmem_limit_bytes=40 * 1024 * 1024
        ),
        cost_estimate=pl.CostEstimate(
            flops=40 * blocks * chunk * rows * width, bytes_accessed=8 * rows * heads * width,
            transcendentals=blocks * chunk * rows,
        ),
    )(gate_row, gate_col, queries, key_rows, values)


def slot_places(route_rows, experts, capacity):
    entries = route_rows.reshape(-1)
    matches = (entries[:, None] == jnp.arange(experts, dtype=jnp.int32)[None, :]).astype(jnp.int32)
    earlier = jnp.cumsum(matches, axis=0) - matches
    ranking = jnp.sum(earlier * matches, axis=1)
    return entries * capacity + ranking


def source_table(places, rows_count, chosen, total_slots):
    owners = jnp.arange(places.shape[0], dtype=jnp.int32) // chosen
    return jnp.full((total_slots,), rows_count, jnp.int32).at[places].set(owners)


def body(
    queries,
    key_rows,
    values,
    forget_log,
    out_weight,
    expert_input,
    norm_gain,
    route_ids,
    route_weights,
    gate_weight,
    up_weight,
    down_weight,
):
    as_float = expert_input.astype(jnp.float32)
    center = jnp.mean(as_float, axis=1, keepdims=True)
    variance = jnp.mean(jnp.square(as_float - center), axis=1, keepdims=True)
    normed = ((as_float - center) * lax.rsqrt(variance + EPSILON) * norm_gain).astype(jnp.bfloat16)
    group_rows = lax.all_gather(normed, "tp", axis=0, tiled=True)
    block_rows = route_ids.shape[0]
    chosen = route_ids.shape[1]
    expert_local = gate_weight.shape[0]
    ep_count = lax.axis_size("ep")
    tp_count = lax.axis_size("tp")
    experts = expert_local * ep_count
    capacity = block_rows * chosen * 2 // experts
    places = slot_places(route_ids, experts, capacity)
    slot_table = source_table(places, block_rows, chosen, experts * capacity).reshape(
        ep_count, expert_local, capacity
    )
    share_size = capacity // tp_count
    part_table = lax.dynamic_slice_in_dim(
        slot_table, lax.axis_index("tp") * share_size, share_size, 2
    )
    outgoing = jnp.take(group_rows, part_table, axis=0, mode="fill", fill_value=0)
    arrived = lax.all_to_all(outgoing, "ep", split_axis=0, concat_axis=0, tiled=True)
    arrived, queries = lax.optimization_barrier((arrived, queries))
    attended = attention(queries, key_rows, values, forget_log)
    arrived_rows = lax.all_gather(arrived, "tp", axis=2, tiled=True)
    arrived_rows, attended = lax.optimization_barrier((arrived_rows, attended))
    gate_part = jnp.einsum(
        "sxcd,xdf->sxcf", arrived_rows, gate_weight, preferred_element_type=jnp.float32
    )
    up_part = jnp.einsum(
        "sxcd,xdf->sxcf", arrived_rows, up_weight, preferred_element_type=jnp.float32
    )
    hidden = (jax.nn.silu(gate_part) * up_part).astype(jnp.bfloat16)
    slots_all = ep_count * expert_local * capacity
    flat_hidden = hidden.reshape(slots_all, hidden.shape[3])
    out_width = out_weight.shape[1]
    mixer_sum = jnp.dot(
        lax.all_gather(attended, "tp", axis=1, tiled=True),
        out_weight,
        preferred_element_type=jnp.float32,
    )
    part_rows = lax.all_gather(flat_hidden, "tp", axis=1, tiled=True)
    shaped = part_rows.reshape(ep_count, expert_local, capacity, part_rows.shape[1])
    product = jnp.einsum("sxcf,xfd->sxcd", shaped, down_weight, preferred_element_type=jnp.float32)
    expert_sum = product.reshape(slots_all, out_width)
    leaving = expert_sum.astype(jnp.bfloat16).reshape(ep_count, expert_local, capacity, out_width)
    returned = lax.all_to_all(leaving, "ep", split_axis=0, concat_axis=0, tiled=True)
    picked = jnp.take(returned.reshape(experts * capacity, out_width), places, axis=0).astype(
        jnp.float32
    )
    combined = jnp.sum(
        (picked * route_weights.reshape(-1)[:, None]).reshape(block_rows, chosen, out_width), axis=1
    )
    return (mixer_sum.astype(jnp.bfloat16), combined.astype(jnp.bfloat16))


def solution(mesh):
    placed = (
        P("ep", "tp"),
        P("ep", "tp"),
        P("ep", "tp"),
        P(None, "tp"),
        P(None, "tp"),
        P(("ep", "tp"), None),
        P(),
        P("ep", None),
        P("ep", None),
        P("ep", None, "tp"),
        P("ep", None, "tp"),
        P("ep", None, "tp"),
    )
    return jax.shard_map(
        body, mesh=mesh, in_specs=placed, out_specs=(P("ep", "tp"), P("ep", "tp")), check_vma=False
    )
```

```python
import functools
import math

import jax
import jax.numpy as jnp
from jax import lax
from jax.experimental import pallas as pl
from jax.experimental.pallas import tpu as pltpu
from jax.sharding import PartitionSpec as P

EPSILON = 1e-05
LOG2E = math.log2(math.e)


def attention_kernel(
    n, tp, heads, gate_row, gate_col, q_ref, k_ref, v_ref, pick_ref, token_ref,
    out_ref, routed_ref,
    k_buf, v_buf, q_buf, o_buf, token_buf, leave_buf,
    recv_k, recv_v, recv_q, recv_o, send_k, send_v, send_q, send_o, pass_k, pass_v,
    send_t, recv_t, send_a, recv_a, send_f, recv_f,
):
    members = n // heads
    rows = k_ref.shape[0]
    width = k_ref.shape[1] // heads
    chunk = rows // members
    me = lax.axis_index("ep")
    my_member = me % members
    my_head = me // members
    my_tp = lax.axis_index("tp")
    tokens = token_ref.shape[0]

    barrier = pltpu.get_barrier_semaphore()

    @pl.loop(1, n)
    def _(step):
        pl.semaphore_signal(barrier, inc=1, device_id={"ep": (me + step) % n})

    @pl.loop(1, tp)
    def _(step):
        pl.semaphore_signal(barrier, inc=1, device_id={"tp": (my_tp + step) % tp})

    pl.semaphore_wait(barrier, n + tp - 2)

    def k_copy(target, head):
        cols = pl.ds(pl.multiple_of(head * width, width), width)
        return pltpu.make_async_remote_copy(
            src_ref=k_ref.at[:, cols], dst_ref=k_buf.at[me], send_sem=send_k.at[head],
            recv_sem=recv_k.at[me], device_id={"ep": target},
        )

    def v_copy(target, head):
        cols = pl.ds(pl.multiple_of(head * width, width), width)
        return pltpu.make_async_remote_copy(
            src_ref=v_ref.at[:, cols], dst_ref=v_buf.at[me], send_sem=send_v.at[head],
            recv_sem=recv_v.at[me], device_id={"ep": target},
        )

    def q_copy(target):
        cols = pl.ds(pl.multiple_of((target // members) * width, width), width)
        part = pl.ds(pl.multiple_of((target % members) * chunk, chunk), chunk)
        return pltpu.make_async_remote_copy(
            src_ref=q_ref.at[part, cols], dst_ref=q_buf.at[me], send_sem=send_q.at[target],
            recv_sem=recv_q.at[me], device_id={"ep": target},
        )

    def pass_copies(source, target):
        return (
            pltpu.make_async_remote_copy(
                src_ref=k_buf.at[source], dst_ref=k_buf.at[source],
                send_sem=pass_k.at[source, target % members],
                recv_sem=recv_k.at[source], device_id={"ep": target},
            ),
            pltpu.make_async_remote_copy(
                src_ref=v_buf.at[source], dst_ref=v_buf.at[source],
                send_sem=pass_v.at[source, target % members],
                recv_sem=recv_v.at[source], device_id={"ep": target},
            ),
        )

    def back_copy(source):
        cols = pl.ds(pl.multiple_of(my_head * width, width), width)
        part = pl.ds(pl.multiple_of(my_member * chunk, chunk), chunk)
        return pltpu.make_async_remote_copy(
            src_ref=o_buf.at[source], dst_ref=out_ref.at[part, cols], send_sem=send_o.at[source],
            recv_sem=recv_o.at[me], device_id={"ep": source},
        )

    def token_spot(owner):
        return token_buf.at[pl.ds(pl.multiple_of(owner * tokens, tokens), tokens), :]

    def token_copy(target):
        return pltpu.make_async_remote_copy(
            src_ref=token_ref, dst_ref=token_spot(my_tp), send_sem=send_t.at[target],
            recv_sem=recv_t.at[my_tp], device_id={"tp": target},
        )

    def leave_copy(target):
        return pltpu.make_async_remote_copy(
            src_ref=leave_buf.at[target], dst_ref=routed_ref.at[me, my_tp],
            send_sem=send_a.at[target], recv_sem=recv_a.at[me], device_id={"ep": target},
        )

    def spread_copy(source, target):
        spot = routed_ref.at[source, my_tp]
        return pltpu.make_async_remote_copy(
            src_ref=spot, dst_ref=spot, send_sem=send_f.at[source, target],
            recv_sem=recv_f.at[source, my_tp], device_id={"tp": target},
        )

    pltpu.make_async_copy(token_ref, token_spot(my_tp), recv_t.at[my_tp]).start()

    @pl.loop(1, tp)
    def _(step):
        token_copy((my_tp + step) % tp).start()

    own_cols = pl.ds(pl.multiple_of(my_head * width, width), width)
    own_part = pl.ds(pl.multiple_of(my_member * chunk, chunk), chunk)
    pltpu.make_async_copy(k_ref.at[:, own_cols], k_buf.at[me], recv_k.at[me]).start()
    pltpu.make_async_copy(v_ref.at[:, own_cols], v_buf.at[me], recv_v.at[me]).start()
    pltpu.make_async_copy(q_ref.at[own_part, own_cols], q_buf.at[me], recv_q.at[me]).start()

    @pl.loop(1, heads)
    def _(step):
        head = (my_head + step) % heads
        k_copy(head * members + my_member, head).start()
        v_copy(head * members + my_member, head).start()

    @pl.loop(1, n)
    def _(step):
        q_copy((me + step) % n).start()

    @pl.loop(0, tp)
    def _(owner):
        pltpu.make_async_copy(token_spot(owner), token_spot(owner), recv_t.at[owner]).wait()

    @pl.loop(0, n)
    def _(target):
        leave_buf[target] = jnp.dot(
            pick_ref[target], token_buf[...], preferred_element_type=jnp.float32
        ).astype(leave_buf.dtype)

    pltpu.make_async_copy(leave_buf.at[me], routed_ref.at[me, my_tp], recv_a.at[me]).start()

    @pl.loop(1, n)
    def _(step):
        leave_copy((me + step) % n).start()

    def landed(source):
        pltpu.make_async_copy(k_buf.at[source], k_buf.at[source], recv_k.at[source]).wait()
        pltpu.make_async_copy(v_buf.at[source], v_buf.at[source], recv_v.at[source]).wait()

    @pl.loop(0, heads)
    def _(step):
        source = ((my_head + step) % heads) * members + my_member
        landed(source)

        @pl.loop(1, members)
        def _(other):
            for copy in pass_copies(source, my_head * members + (my_member + other) % members):
                copy.start()

    column = lax.broadcasted_iota(jnp.int32, (chunk, rows), 1)
    line = lax.broadcasted_iota(jnp.int32, (chunk, rows), 0) + my_member * chunk
    causal = column <= line
    factor = LOG2E * width ** (-0.5)

    @pl.loop(0, n)
    def _(i):
        pltpu.make_async_copy(q_buf.at[i], q_buf.at[i], recv_q.at[i]).wait()

        @pl.when(i % members != my_member)
        def _():
            landed(i)

        query = q_buf[i]
        line_gate = gate_col[i]

        def scores_of(j):
            raw = lax.dot_general(
                query, k_buf[j], (((1,), (1,)), ((), ())), preferred_element_type=jnp.float32
            )
            return raw * factor + (line_gate - gate_row[j])

        def weigh(weights, j):
            return jnp.dot(
                weights.astype(jnp.bfloat16), v_buf[j], preferred_element_type=jnp.float32
            )

        scores = jnp.where(causal, scores_of(i), -jnp.inf)
        top = jnp.max(scores, axis=1, keepdims=True)
        weights = jnp.exp2(scores - top)
        total = jnp.sum(weights, axis=1, keepdims=True)
        held = weigh(weights, i)

        def fold(j, state):
            top, total, held = state
            scores = scores_of(j)
            newest = jnp.maximum(top, jnp.max(scores, axis=1, keepdims=True))
            shrink = jnp.exp2(top - newest)
            weights = jnp.exp2(scores - newest)
            total = total * shrink + jnp.sum(weights, axis=1, keepdims=True)
            held = held * shrink + weigh(weights, j)
            return newest, total, held

        top, total, held = lax.fori_loop(0, i, fold, (top, total, held))
        o_buf[i] = (held / total).astype(o_buf.dtype)

        @pl.when(i != me)
        def _():
            back_copy(i).start()

        source = (me + n - i) % n
        spot = routed_ref.at[source, my_tp]
        pltpu.make_async_copy(spot, spot, recv_a.at[source]).wait()

        @pl.loop(1, tp)
        def _(step):
            spread_copy(source, (my_tp + step) % tp).start()

    own = pltpu.make_async_copy(o_buf.at[me], out_ref.at[own_part, own_cols], recv_o.at[me])
    own.start()

    @pl.loop(1, heads)
    def _(step):
        head = (my_head + step) % heads
        k_copy(head * members + my_member, head).wait_send()
        v_copy(head * members + my_member, head).wait_send()

    @pl.loop(1, n)
    def _(step):
        q_copy((me + step) % n).wait_send()
        back_copy((me + step) % n).wait_send()
        leave_copy((me + step) % n).wait_send()

    @pl.loop(1, tp)
    def _(step):
        token_copy((my_tp + step) % tp).wait_send()

    @pl.loop(0, n)
    def _(source):
        @pl.loop(1, tp)
        def _(step):
            other = (my_tp + step) % tp
            spread_copy(source, other).wait_send()
            spot = routed_ref.at[source, other]
            pltpu.make_async_copy(spot, spot, recv_f.at[source, other]).wait()

    @pl.loop(0, heads)
    def _(step):
        source = step * members + my_member

        @pl.loop(1, members)
        def _(other):
            for copy in pass_copies(source, my_head * members + (my_member + other) % members):
                copy.wait_send()

    @pl.loop(0, n)
    def _(i):
        cols = pl.ds(pl.multiple_of((i // members) * width, width), width)
        part = pl.ds(pl.multiple_of((i % members) * chunk, chunk), chunk)
        spot = out_ref.at[part, cols]
        pltpu.make_async_copy(spot, spot, recv_o.at[i]).wait()


def attention(queries, key_rows, values, forget_log, picks, normed):
    n, tp = lax.axis_size("ep"), lax.axis_size("tp")
    share, depth = picks.shape[1], normed.shape[1]
    rows, heads = queries.shape[0], forget_log.shape[1]
    width = queries.shape[1] // heads
    members = n // heads
    chunk = rows // members
    me = lax.axis_index("ep")
    gates = lax.dynamic_slice_in_dim(forget_log.T * LOG2E, me // members, 1, 0)
    gate_row = gates.reshape(n, 1, rows)
    gate_col = lax.dynamic_slice_in_dim(
        gates.reshape(n, members, chunk), me % members, 1, 1
    ).reshape(n, chunk, 1)
    vmem = pl.BlockSpec(memory_space=pltpu.VMEM)
    dma = pltpu.SemaphoreType.DMA
    blocks = n * (n + 1) // 2
    return pl.pallas_call(
        functools.partial(attention_kernel, n, tp, heads),
        out_shape=(
            jax.ShapeDtypeStruct((rows, heads * width), jnp.bfloat16),
            jax.ShapeDtypeStruct((n, tp, share, depth), jnp.bfloat16),
        ),
        in_specs=[vmem] * 7,
        out_specs=(vmem, vmem),
        scratch_shapes=[
            pltpu.VMEM((n, rows, width), jnp.bfloat16),
            pltpu.VMEM((n, rows, width), jnp.bfloat16),
            pltpu.VMEM((n, chunk, width), jnp.bfloat16),
            pltpu.VMEM((n, chunk, width), jnp.bfloat16),
            pltpu.VMEM((tp * normed.shape[0], depth), jnp.bfloat16),
            pltpu.VMEM((n, share, depth), jnp.bfloat16),
            dma((n,)), dma((n,)), dma((n,)), dma((n,)),
            dma((heads,)), dma((heads,)), dma((n,)), dma((n,)),
            dma((n, members)), dma((n, members)),
            dma((tp,)), dma((tp,)), dma((n,)), dma((n,)), dma((n, tp)), dma((n, tp)),
        ],
        compiler_params=pltpu.CompilerParams(
            collective_id=0, has_side_effects=True, vmem_limit_bytes=40 * 1024 * 1024
        ),
        cost_estimate=pl.CostEstimate(
            flops=40 * blocks * chunk * rows * width, bytes_accessed=8 * rows * heads * width,
            transcendentals=blocks * chunk * rows,
        ),
    )(gate_row, gate_col, queries, key_rows, values, picks, normed)


def slot_places(route_rows, experts, capacity):
    entries = route_rows.reshape(-1)
    matches = (entries[:, None] == jnp.arange(experts, dtype=jnp.int32)[None, :]).astype(jnp.int32)
    earlier = jnp.cumsum(matches, axis=0) - matches
    ranking = jnp.sum(earlier * matches, axis=1)
    return entries * capacity + ranking


def body(
    queries,
    key_rows,
    values,
    forget_log,
    out_weight,
    expert_input,
    norm_gain,
    route_ids,
    route_weights,
    gate_weight,
    up_weight,
    down_weight,
):
    as_float = expert_input.astype(jnp.float32)
    center = jnp.mean(as_float, axis=1, keepdims=True)
    variance = jnp.mean(jnp.square(as_float - center), axis=1, keepdims=True)
    normed = ((as_float - center) * lax.rsqrt(variance + EPSILON) * norm_gain).astype(jnp.bfloat16)
    block_rows = route_ids.shape[0]
    chosen = route_ids.shape[1]
    expert_local = gate_weight.shape[0]
    ep_count = lax.axis_size("ep")
    tp_count = lax.axis_size("tp")
    experts = expert_local * ep_count
    capacity = block_rows * chosen * 2 // experts
    places = slot_places(route_ids, experts, capacity)
    share_size = capacity // tp_count
    own_slots = lax.axis_index("tp") * share_size + jnp.arange(share_size, dtype=jnp.int32)
    part_slots = jnp.arange(experts, dtype=jnp.int32)[:, None] * capacity + own_slots[None, :]
    picks = jnp.any(
        part_slots.reshape(ep_count, expert_local * share_size)[:, :, None, None]
        == places.reshape(block_rows, chosen).T[None, None, :, :],
        axis=2,
    ).astype(jnp.bfloat16)
    attended, routed = attention(queries, key_rows, values, forget_log, picks, normed)
    arrived_rows = (
        routed.reshape(ep_count, tp_count, expert_local, share_size, routed.shape[3])
        .transpose(0, 2, 1, 3, 4)
        .reshape(ep_count, expert_local, capacity, routed.shape[3])
    )
    gate_part = jnp.einsum(
        "sxcd,xdf->sxcf", arrived_rows, gate_weight, preferred_element_type=jnp.float32
    )
    up_part = jnp.einsum(
        "sxcd,xdf->sxcf", arrived_rows, up_weight, preferred_element_type=jnp.float32
    )
    hidden = (jax.nn.silu(gate_part) * up_part).astype(jnp.bfloat16)
    slots_all = ep_count * expert_local * capacity
    flat_hidden = hidden.reshape(slots_all, hidden.shape[3])
    out_width = out_weight.shape[1]
    mixer_sum = jnp.dot(
        lax.all_gather(attended, "tp", axis=1, tiled=True),
        out_weight,
        preferred_element_type=jnp.float32,
    )
    part_rows = lax.all_gather(flat_hidden, "tp", axis=1, tiled=True)
    shaped = part_rows.reshape(ep_count, expert_local, capacity, part_rows.shape[1])
    product = jnp.einsum("sxcf,xfd->sxcd", shaped, down_weight, preferred_element_type=jnp.float32)
    expert_sum = product.reshape(slots_all, out_width)
    leaving = expert_sum.astype(jnp.bfloat16).reshape(ep_count, expert_local, capacity, out_width)
    returned = lax.all_to_all(leaving, "ep", split_axis=0, concat_axis=0, tiled=True)
    picked = jnp.take(returned.reshape(experts * capacity, out_width), places, axis=0).astype(
        jnp.float32
    )
    combined = jnp.sum(
        (picked * route_weights.reshape(-1)[:, None]).reshape(block_rows, chosen, out_width), axis=1
    )
    return (mixer_sum.astype(jnp.bfloat16), combined.astype(jnp.bfloat16))


def solution(mesh):
    placed = (
        P("ep", "tp"),
        P("ep", "tp"),
        P("ep", "tp"),
        P(None, "tp"),
        P(None, "tp"),
        P(("ep", "tp"), None),
        P(),
        P("ep", None),
        P("ep", None),
        P("ep", None, "tp"),
        P("ep", None, "tp"),
        P("ep", None, "tp"),
    )
    return jax.shard_map(
        body, mesh=mesh, in_specs=placed, out_specs=(P("ep", "tp"), P("ep", "tp")), check_vma=False
    )
```
